32 devices in a mesh: sp: 4 (over z), fs: 4 (over y, x), tp: 2 (over core).
Axes of the slice: x: 2, y: 2, z: 4, core: 2. Of those that a mesh axis runs over, the one named last changes fastest.
Arguments:
- tokens: bfloat16 [4, 1024, 2048], P('fs', 'sp', 'tp'), may hold values from -6 to 6
- norm_gain: float32 [2048], replicated, may hold values from 0.1 to 1.9
- w_query: bfloat16 [2048, 1024], P(('sp', 'fs'), 'tp'), may hold values from -0.125 to 0.125
- forget_weight: bfloat16 [2048, 1024], P(('sp', 'fs'), 'tp'), may hold values from -0.125 to 0.125
- w_input: bfloat16 [2048, 1024], P(('sp', 'fs'), 'tp'), may hold values from -8 to 8
- w_outgate: bfloat16 [2048, 1024], P(('sp', 'fs'), 'tp'), may hold values from -0.125 to 0.125
- w_pool: bfloat16 [2048, 1024], P(('sp', 'fs'), 'tp'), may hold values from -0.125 to 0.125
- forget_gap: float32 [1024], P('tp'), may hold values from 0 to 0.07
- extra_decay: float32 [4, 1024, 8], P('fs', 'sp', 'tp'), may hold values from -0.61 to 0
- rec_gain: float32 [1024], P('tp'), may hold values from 0.1 to 1.9
- group_weight: bfloat16 [4, 256, 256], replicated, may hold values from -0.375 to 0.375
- pool_gain: float32 [1024], P('tp'), may hold values from 0.1 to 1.9
- recurrent_output_weight: bfloat16 [1024, 2048], P('tp', ('sp', 'fs')), may hold values from -0.1875 to 0.1875
- w_out_pool: bfloat16 [1024, 2048], P('tp', ('sp', 'fs')), may hold values from -0.1875 to 0.1875
Outputs:
- mixed_out: bfloat16 [4, 1024, 2048], P('fs', ('sp', 'tp'))
The draws below stay inside these ranges and needn't reach their ends.
All inputs are finite; a program needn't handle non-finite values.
Results may differ from the reference program's by a relative error of at most 0.011.
Values may be sent and summed in bfloat16 or wider, within the bound.
No kernel may reach another device: no remote copies, remote signals or barrier semaphores. Data moves between devices by JAX's collectives and lax.ppermute only.
A program may use at most 64 MiB of HBM per device.

```python
import math
import jax
import jax.numpy as jnp
from jax import lax

D = 2048
HGRN_HEADS = 8
HEAD_DIM = 128
D_HGRN = 1024
D_POOL = 1024
POOL_GROUPS = 4
GROUP_DIM = 256
BLOCK = 64
TOK_DEV = 256
SEQ_LEN = 1024
SEQS = 4
N_TP = 2


def head_speeds(key):
    order = jax.random.permutation(jax.random.fold_in(key, 17), HGRN_HEADS)
    fast_count = HGRN_HEADS // 2
    return order < fast_count


def draw_forget_gap(key, part):
    fast_heads = head_speeds(key)
    spread = jax.random.uniform(jax.random.fold_in(key, 5), (HGRN_HEADS, HEAD_DIM), jnp.float32)
    fast_gap = 0.025 * jnp.exp(spread * math.log(2.8))
    slow_gap = 0.3 * jnp.exp(spread * math.log(4.0)) / SEQ_LEN
    return jnp.where(fast_heads[:, None], fast_gap, slow_gap).reshape(D_HGRN).astype(jnp.float32)


def draw_w_input(key, part):
    fast_heads = head_speeds(key)
    normal_draw = jnp.clip(jax.random.normal(jax.random.fold_in(key, 3), (D, D_HGRN), jnp.float32), -6.0, 6.0)
    slow_scale = math.sqrt(SEQ_LEN) / 4.0
    column_scale = jnp.repeat(jnp.where(fast_heads, 1.0, slow_scale), HEAD_DIM)
    return (normal_draw * column_scale[None, :] / math.sqrt(D)).astype(jnp.bfloat16)


def draw_extra_decay(key, part):
    base_key = jax.random.fold_in(key, 9)
    rate_key, spot_key, depth_key = jax.random.split(base_key, 3)
    block_total = SEQ_LEN // TOK_DEV
    level = jax.random.uniform(rate_key, (SEQS, block_total, 1, HGRN_HEADS), jnp.float32)
    shrink_factor_list = 0.15 * jnp.exp(level * math.log(4.0)) / SEQ_LEN
    shrink_factor_list = jnp.broadcast_to(shrink_factor_list, (SEQS, block_total, TOK_DEV, HGRN_HEADS)).reshape(SEQS, SEQ_LEN, HGRN_HEADS)
    first_spot = jax.random.randint(jax.random.fold_in(spot_key, 1), (SEQS, 1, HGRN_HEADS, 1), 0, SEQ_LEN)
    spot_offset = jax.random.randint(jax.random.fold_in(spot_key, 2), (SEQS, 1, HGRN_HEADS, 1), 1, SEQ_LEN)
    second_spot = (first_spot + spot_offset) % SEQ_LEN
    probe_locations = jnp.concatenate([first_spot, second_spot], axis=3)
    layer_tiers = jnp.log(0.55 + 0.25 * jax.random.uniform(depth_key, (SEQS, 1, HGRN_HEADS, 2), jnp.float32))
    symbol_indices = jnp.arange(SEQ_LEN, dtype=jnp.int32)[None, :, None, None]
    spike_clusters = jnp.sum(jnp.where(symbol_indices == probe_locations, layer_tiers, 0.0), axis=3)
    return (spike_clusters - shrink_factor_list).astype(jnp.float32)


def level_of(key, dims, cuts, smallest, largest):
    gain = 1.0
    for axis_at, shards_of in cuts:
        draws = jax.random.uniform(jax.random.fold_in(jax.random.fold_in(key, 6), axis_at), (shards_of,), jnp.float32, smallest / len(cuts), largest / len(cuts))
        gain = gain * jnp.repeat(jnp.exp(draws), dims[axis_at] // shards_of).reshape((-1,) + (1,) * (len(dims) - 1 - axis_at))
    return gain


def noise(key, extent, scale, bound, cuts=(), held_as=jnp.bfloat16):
    drawn = jax.random.normal(key, extent, jnp.float32) * scale
    if len(cuts) > 0:
        drawn = level_of(key, extent, cuts, -0.22, 0.18) * drawn
    return jnp.clip(drawn, min=-bound, max=bound).astype(held_as)


def setup_inputs(seed: int = 0) -> dict:
    key_list = jax.random.split(jax.random.key(seed), 15)
    return {
        "tokens": noise(key_list[0], (SEQS, SEQ_LEN, D), 1.0, 6.0, ((0, 4), (1, 4), (2, 2))),
        "norm_gain": jnp.clip(1.0 + 0.18 * jax.random.normal(key_list[1], (D,), jnp.float32), 0.1, 1.9),
        "w_query": noise(key_list[2], (D, D_HGRN), D ** -0.5, 0.125, ((0, 16), (1, 2))),
        "forget_weight": noise(key_list[3], (D, D_HGRN), D ** -0.5, 0.125, ((0, 16), (1, 2))),
        "w_input": draw_w_input(jax.random.fold_in(key_list[14], 71), 0),
        "w_outgate": noise(key_list[5], (D, D_HGRN), D ** -0.5, 0.125, ((0, 16), (1, 2))),
        "w_pool": noise(key_list[6], (D, D_POOL), D ** -0.5, 0.125, ((0, 16), (1, 2))),
        "forget_gap": draw_forget_gap(jax.random.fold_in(key_list[14], 71), 0),
        "extra_decay": draw_extra_decay(jax.random.fold_in(key_list[14], 71), 0),
        "rec_gain": jnp.clip(1.0 + 0.18 * jax.random.normal(key_list[9], (D_HGRN,), jnp.float32), 0.1, 1.9),
        "group_weight": noise(key_list[10], (POOL_GROUPS, GROUP_DIM, GROUP_DIM), GROUP_DIM ** -0.5, 0.375),
        "pool_gain": jnp.clip(1.0 + 0.18 * jax.random.normal(key_list[11], (D_POOL,), jnp.float32), 0.1, 1.9),
        "recurrent_output_weight": noise(key_list[12], (D_HGRN, D), D_HGRN ** -0.5, 0.1875, ((0, 2), (1, 16))),
        "w_out_pool": noise(key_list[13], (D_POOL, D), D_POOL ** -0.5, 0.1875, ((0, 2), (1, 16))),
    }


EPS = 1e-06
HIGH = lax.Precision.HIGHEST

def recurrence(queries, input_gate, values, log_forget):
    block_count = queries.shape[0] // BLOCK
    shaped = tuple((arr.reshape(block_count, BLOCK, HGRN_HEADS, HEAD_DIM) for arr in (queries, input_gate, values, log_forget)))
    causal = jnp.tril(jnp.ones((BLOCK, BLOCK), jnp.bool_))

    def advance(carried, pieces):
        q_blk, k_blk, v_blk, g_blk = pieces
        within = jnp.cumsum(g_blk, axis=0)
        block_end = within[-1]
        q_up = q_blk * jnp.exp(within)
        scores = jnp.einsum('thd,shd->hts', q_up, k_blk * jnp.exp(-within), precision=HIGH)
        scores = jnp.where(causal, scores, 0.0)
        result = jnp.einsum('hts,she->the', scores, v_blk, precision=HIGH)
        result = result + jnp.einsum('thd,hde->the', q_up, carried, precision=HIGH)
        fresh_input = jnp.einsum('shd,she->hde', k_blk * jnp.exp(block_end[None] - within), v_blk, precision=HIGH)
        carried = jnp.exp(block_end)[:, :, None] * carried + fresh_input
        return (carried, result)
    initial = jnp.zeros((HGRN_HEADS, HEAD_DIM, HEAD_DIM), jnp.float32)
    _, results = lax.scan(advance, initial, shaped)
    return results.reshape(queries.shape[0], D_HGRN)

def pooling(z_pool, group_weight, pool_gain):
    seq_rows = z_pool.shape[0]
    reach_rows = 2 ** POOL_GROUPS
    values = z_pool.astype(jnp.float32)
    padded = jnp.pad(values, ((reach_rows, 0), (0, 0)))
    symbol_indices = jnp.arange(seq_rows, dtype=jnp.int32)
    outputs = []
    for group_idx in range(POOL_GROUPS):
        window_len = 2 ** (group_idx + 1)
        lowest_column_index = group_idx * GROUP_DIM
        high_col = lowest_column_index + GROUP_DIM
        window = padded[reach_rows:reach_rows + seq_rows, lowest_column_index:high_col]
        for shift_idx in range(1, window_len):
            window = window + padded[reach_rows - shift_idx:reach_rows - shift_idx + seq_rows, lowest_column_index:high_col]
        counts_here = jnp.minimum(symbol_indices + 1, window_len).astype(jnp.float32)[:, None]
        pooled = (window / counts_here - values[:, lowest_column_index:high_col]).astype(jnp.bfloat16)
        mapped = jnp.dot(pooled, group_weight[group_idx], preferred_element_type=jnp.float32)
        outputs.append((mapped * pool_gain[lowest_column_index:high_col]).astype(jnp.bfloat16))
    return jnp.concatenate(outputs, axis=1)

def one_sequence(tokens_seq, extra_seq, weights):
    norm_gain, w_query, forget_weight, w_input, w_outgate, w_pool, forget_gap, rec_gain, group_weight, pool_gain, recurrent_output_weight, w_out_pool = weights
    features_f = tokens_seq.astype(jnp.float32)
    token_scale = lax.rsqrt(lax.optimization_barrier(jnp.mean(features_f * features_f, axis=-1, keepdims=True)) + EPS)
    normed = (features_f * token_scale * norm_gain).astype(jnp.bfloat16)

    def project(matrix):
        return jnp.dot(normed, matrix, preferred_element_type=jnp.float32).astype(jnp.bfloat16)
    z_query = project(w_query)
    z_forget = project(forget_weight)
    z_input = project(w_input)
    z_outgate = project(w_outgate)
    z_pool = project(w_pool)
    input_gate = forget_gap * jax.nn.sigmoid(-z_forget.astype(jnp.float32))
    log_forget = jnp.log1p(-input_gate) + jnp.repeat(extra_seq, HEAD_DIM, axis=1)
    queries = jax.nn.silu(z_query.astype(jnp.float32))
    recurrent = recurrence(queries, input_gate, z_input.astype(jnp.float32), log_forget)
    rec_scale = lax.rsqrt(lax.optimization_barrier(jnp.mean(recurrent * recurrent, axis=-1, keepdims=True)) + EPS)
    recurrent_output = (recurrent * rec_scale * rec_gain * jax.nn.silu(z_outgate.astype(jnp.float32))).astype(jnp.bfloat16)
    pool_out = pooling(z_pool, group_weight, pool_gain)
    rec_rows = D_HGRN // N_TP
    pool_rows = D_POOL // N_TP
    summed_out = jnp.zeros((tokens_seq.shape[0], D), jnp.float32)
    for block_idx in range(N_TP):
        rec_lo = block_idx * rec_rows
        pool_lo = block_idx * pool_rows
        partial_sum = jnp.dot(recurrent_output[:, rec_lo:rec_lo + rec_rows], recurrent_output_weight[rec_lo:rec_lo + rec_rows], preferred_element_type=jnp.float32) + jnp.dot(pool_out[:, pool_lo:pool_lo + pool_rows], w_out_pool[pool_lo:pool_lo + pool_rows], preferred_element_type=jnp.float32)
        rounded = lax.optimization_barrier(partial_sum.astype(jnp.bfloat16))
        summed_out = summed_out + rounded.astype(jnp.float32)
    return summed_out.astype(jnp.bfloat16)

def reference(tokens, norm_gain, w_query, forget_weight, w_input, w_outgate, w_pool, forget_gap, extra_decay, rec_gain, group_weight, pool_gain, recurrent_output_weight, w_out_pool):
    weights = (norm_gain, w_query, forget_weight, w_input, w_outgate, w_pool, forget_gap, rec_gain, group_weight, pool_gain, recurrent_output_weight, w_out_pool)

    def per_sequence(pair):
        return one_sequence(pair[0], pair[1], weights)
    return lax.map(per_sequence, (tokens, extra_decay))
```

```python
import jax
import jax.numpy as jnp
from jax import lax
from jax.experimental import pallas as pl
from jax.experimental.pallas import tpu as pltpu
from jax.sharding import PartitionSpec as P

HEAD_DIM = 128
D_HGRN = 1024
POOL_GROUPS = 4
GROUP_DIM = 256
BLOCK = 64


EPS = 1e-06
HIGH = lax.Precision.HIGHEST


def carried_in(x, axis, join, neutral):
    place = lax.axis_index(axis)
    gathered = jax.tree.map(
        lambda a, kind: lax.all_gather(a.astype(kind), axis), x, (jnp.bfloat16, jnp.bfloat16)
    )
    state = jax.tree.map(lambda a, e: jnp.zeros_like(a) + jnp.asarray(e, a.dtype), x, neutral)

    def one(lap, state):
        return join(
            state,
            jax.tree.map(
                lambda a, own: lax.dynamic_index_in_dim(a, lap, 0, False).astype(own.dtype),
                gathered,
                x,
            ),
        )

    return lax.fori_loop(0, place, one, state)


def shifted(x, axis, by):
    peers = lax.axis_size(axis)
    pairs = [(i, i + by) for i in range(peers) if 0 <= i + by < peers]
    return lax.ppermute(x, axis, pairs)


def local_recurrence(queries, input_gate, values, log_forget):
    tok_rows, head_count = (queries.shape[0], queries.shape[1])
    block_count = tok_rows // BLOCK
    q_blk, k_blk, v_blk, g_blk = (
        arr.reshape(block_count, BLOCK, head_count, HEAD_DIM)
        for arr in (queries, input_gate, values, log_forget)
    )
    within = jnp.cumsum(g_blk, axis=1)
    block_end = within[:, -1]
    q_up = q_blk * jnp.exp(within)
    k_down = k_blk * jnp.exp(-within)
    causal = jnp.tril(jnp.ones((BLOCK, BLOCK), jnp.bool_))
    scores = jnp.einsum("nthd,nshd->nhts", q_up, k_down, precision=HIGH)
    scores = jnp.where(causal, scores, 0.0)
    inner_out = jnp.einsum("nhts,nshe->nthe", scores, v_blk, precision=HIGH)
    updates = jnp.einsum(
        "nshd,nshe->nhde", k_blk * jnp.exp(block_end[:, None] - within), v_blk, precision=HIGH
    )
    decays = jnp.exp(block_end)

    def carry_step(carried_state, step_inputs):
        current_shrink_factor, update_now = step_inputs
        return (current_shrink_factor[:, :, None] * carried_state + update_now, carried_state)

    zero_state = jnp.zeros((head_count, HEAD_DIM, HEAD_DIM), jnp.float32)
    final_state, incoming = lax.scan(carry_step, zero_state, (decays, updates))
    local_out = inner_out + jnp.einsum("nthd,nhde->nthe", q_up, incoming, precision=HIGH)
    offsets = jnp.cumsum(block_end, axis=0) - block_end
    total_log = jnp.sum(block_end, axis=0)
    query_dev = q_up * jnp.exp(offsets[:, None])
    return (local_out, final_state, total_log, query_dev)


def combine_states(earlier, later):
    decay_early, state_early = earlier
    decay_late, state_late = later
    return (decay_early * decay_late, decay_late[:, :, None] * state_early + state_late)


def body(
    tokens,
    norm_gain,
    w_query,
    forget_weight,
    w_input,
    w_outgate,
    w_pool,
    forget_gap,
    extra_decay,
    rec_gain,
    group_weight,
    pool_gain,
    recurrent_output_weight,
    w_out_pool,
):
    gathered = lax.all_gather(tokens[0], "tp", axis=1, tiled=True)
    features_f = gathered.astype(jnp.float32)
    token_scale = lax.rsqrt(jnp.mean(features_f * features_f, axis=-1, keepdims=True) + EPS)
    normed = (features_f * token_scale * norm_gain).astype(jnp.bfloat16)
    tok_rows = normed.shape[0]
    width_dev = w_query.shape[1]
    pool_dev = w_pool.shape[1]
    near_rows = (
        lax.all_gather(w_query, "fs", axis=0, tiled=True),
        lax.all_gather(forget_weight, "fs", axis=0, tiled=True),
        lax.all_gather(w_input, "fs", axis=0, tiled=True),
        lax.all_gather(w_outgate, "fs", axis=0, tiled=True),
        lax.all_gather(w_pool, "fs", axis=0, tiled=True),
    )
    full_rows = (
        lax.all_gather(near_rows[0], "sp", axis=0, tiled=True),
        lax.all_gather(near_rows[1], "sp", axis=0, tiled=True),
        lax.all_gather(near_rows[2], "sp", axis=0, tiled=True),
        lax.all_gather(near_rows[3], "sp", axis=0, tiled=True),
        lax.all_gather(near_rows[4], "sp", axis=0, tiled=True),
    )
    z_query, z_forget, z_input, z_outgate, z_pool = (
        jnp.dot(normed, matrix, preferred_element_type=jnp.float32).astype(jnp.bfloat16)
        for matrix in full_rows
    )
    heads_dev = width_dev // HEAD_DIM
    input_gate = forget_gap * jax.nn.sigmoid(-z_forget.astype(jnp.float32))
    log_forget = (
        jnp.log1p(-input_gate).reshape(tok_rows, heads_dev, HEAD_DIM) + extra_decay[0][:, :, None]
    )
    queries = jax.nn.silu(z_query.astype(jnp.float32)).reshape(tok_rows, heads_dev, HEAD_DIM)
    values = z_input.astype(jnp.float32).reshape(tok_rows, heads_dev, HEAD_DIM)
    local_out, end_state, total_log, query_dev = local_recurrence(
        queries, input_gate.reshape(tok_rows, heads_dev, HEAD_DIM), values, log_forget
    )
    identity = (jnp.ones_like(total_log), jnp.zeros_like(end_state))
    scanned = carried_in((jnp.exp(total_log), end_state), "sp", combine_states, identity)
    incoming = scanned[1]
    carried = jnp.einsum("nthd,hde->nthe", query_dev, incoming, precision=HIGH)
    recurrent = (local_out + carried).reshape(tok_rows, width_dev)
    square_sum = lax.psum(jnp.sum(recurrent * recurrent, axis=1), "tp")
    rec_scale = lax.rsqrt(square_sum / D_HGRN + EPS)[:, None]
    recurrent_output = (
        recurrent * rec_scale * rec_gain * jax.nn.silu(z_outgate.astype(jnp.float32))
    ).astype(jnp.bfloat16)
    reach_rows = 2**POOL_GROUPS
    rim_rows = shifted(z_pool[tok_rows - reach_rows :], "sp", 1)
    extended = jnp.concatenate([rim_rows, z_pool], axis=0).astype(jnp.float32)
    running = extended
    window_sums = []
    for level_idx in range(POOL_GROUPS):
        stride = 2**level_idx
        running = running[stride:] + running[:-stride]
        window_sums.append(running[running.shape[0] - tok_rows :])
    groups_dev = pool_dev // GROUP_DIM
    stacked = jnp.stack(window_sums).reshape(POOL_GROUPS, tok_rows, groups_dev, GROUP_DIM)
    group_ids = lax.axis_index("tp") * groups_dev + jnp.arange(groups_dev, dtype=jnp.int32)
    chosen = jnp.arange(POOL_GROUPS, dtype=jnp.int32)[:, None] == group_ids[None, :]
    window_total = jnp.sum(jnp.where(chosen[:, None, :, None], stacked, 0.0), axis=0)
    symbol_indices = lax.axis_index("sp") * tok_rows + jnp.arange(tok_rows, dtype=jnp.int32)
    window_len = jnp.left_shift(jnp.int32(2), group_ids)
    counts_here = jnp.minimum(symbol_indices[:, None] + 1, window_len[None, :]).astype(jnp.float32)
    pooled = (
        window_total / counts_here[:, :, None]
        - z_pool.astype(jnp.float32).reshape(tok_rows, groups_dev, GROUP_DIM)
    ).astype(jnp.bfloat16)
    local_weight = lax.dynamic_slice_in_dim(
        group_weight, lax.axis_index("tp") * groups_dev, groups_dev, 0
    )
    mapped = jnp.einsum("tcd,cde->tce", pooled, local_weight, preferred_element_type=jnp.float32)
    pool_out = (mapped.reshape(tok_rows, pool_dev) * pool_gain).astype(jnp.bfloat16)
    rec_columns, pool_columns = (
        lax.all_gather(recurrent_output_weight, ("sp", "fs"), axis=1, tiled=True),
        lax.all_gather(w_out_pool, ("sp", "fs"), axis=1, tiled=True),
    )
    mixed = lax.psum_scatter(
        (
            jnp.dot(recurrent_output, rec_columns, preferred_element_type=jnp.float32)
            + jnp.dot(pool_out, pool_columns, preferred_element_type=jnp.float32)
        ).astype(jnp.bfloat16),
        "tp",
        scatter_dimension=0,
        tiled=True,
    )
    return mixed[None]


F32 = jnp.float32
BF16 = jnp.bfloat16
VMEM = pl.BlockSpec(memory_space=pltpu.VMEM)
SMEM = pl.BlockSpec(memory_space=pltpu.SMEM)
ANY = pl.BlockSpec(memory_space=pl.ANY)
LAST = (((1,), (1,)), ((), ()))
FIRST = (((0,), (0,)), ((), ()))
PLAIN = (((1,), (0,)), ((), ()))


def exact_dot(a, b, dims=PLAIN):
    return lax.dot_general(a, b, dims, precision=HIGH, preferred_element_type=F32)


def dot(a, b):
    return lax.dot_general(a, b, PLAIN, preferred_element_type=F32)


def split_kernel(at, *refs):
    mats, outs = refs[: len(refs) - N_LINE], refs[len(refs) - N_LINE :]
    for d in range(N_LINE):
        head = pl.multiple_of(lax.rem(at[0] + d, N_LINE) * HEAD_DIM, HEAD_DIM)
        for i, mat in enumerate(mats):
            outs[d][:, i * HEAD_DIM : (i + 1) * HEAD_DIM] = mat[:, pl.ds(head, HEAD_DIM)]


def place_kernel(at, *refs):
    pieces, out, sems = refs[:-2], refs[-2], refs[-1]
    rows = pieces[0].shape[-2]
    copies = []
    for e, piece in enumerate(pieces):
        for d in range(N_LINE):
            k = at[e * N_LINE + d]
            copies.append(
                pltpu.make_async_copy(
                    piece.at[d], out.at[pl.ds(k * rows, rows)], sems.at[e * N_LINE + d]
                )
            )
    for c in copies:
        c.start()
    for c in copies:
        c.wait()


def block_kernel(at, own, other, gain, weight, gap, decay, rec_gain, *refs):
    local, query, end, total, gate_out, pool_in = refs[-6:]
    half = own.shape[1]
    a, b = own[...].astype(F32), other[...].astype(F32)
    mean = (
        jnp.sum(a * a, axis=1, keepdims=True) + jnp.sum(b * b, axis=1, keepdims=True)
    ) / (2 * half)
    scale = lax.rsqrt(mean + EPS)
    na = (a * scale * gain[0:1, :]).astype(BF16)
    nb = (b * scale * gain[1:2, :]).astype(BF16)
    z = (dot(na, weight[0:half, :]) + dot(nb, weight[half:, :])).astype(BF16).astype(F32)
    zq, zf, zi, zo, zp = (z[:, i * HEAD_DIM : (i + 1) * HEAD_DIM] for i in range(5))
    rows = z.shape[0]
    keys = gap[...] / (1.0 + jnp.exp(zf))
    log_forget = jnp.log1p(-keys) + decay[...]
    q = zq / (1.0 + jnp.exp(-zq))
    gate_out[0] = rec_gain[...] * (zo / (1.0 + jnp.exp(-zo)))
    pool_in[0] = zp
    t = lax.broadcasted_iota(jnp.int32, (rows, rows), 0)
    s = lax.broadcasted_iota(jnp.int32, (rows, rows), 1)
    causal = (s <= t) & (s // BLOCK == t // BLOCK)
    within = exact_dot(causal.astype(F32), log_forget)
    q_up = q * jnp.exp(within)
    k_down = keys * jnp.exp(-within)
    scores = jnp.where(causal, exact_dot(q_up, k_down, LAST), 0.0)
    inner = exact_dot(scores, zi)
    state = None
    offset = jnp.zeros((1, HEAD_DIM), F32)
    for c in range(rows // BLOCK):
        at_rows = slice(c * BLOCK, (c + 1) * BLOCK)
        w_c, q_c = within[at_rows], q_up[at_rows]
        end_c = w_c[BLOCK - 1 : BLOCK]
        fresh = exact_dot(zi[at_rows], keys[at_rows] * jnp.exp(end_c - w_c), FIRST)
        query[0, at_rows] = q_c * jnp.exp(offset)
        if state is None:
            local[0, at_rows] = inner[at_rows]
            state = fresh
        else:
            local[0, at_rows] = inner[at_rows] + exact_dot(q_c, state, LAST)
            state = state * jnp.exp(end_c) + fresh
        offset = offset + end_c
    end[0] = state
    total[0] = jnp.broadcast_to(offset, total.shape[1:])


def join_kernel(at, local, query, end, total, gate_out, pool_in, *refs):
    outs, pay = refs[:-1], refs[-1]
    blocks, rows, _ = local.shape
    state = None
    for b in range(blocks):
        rec = local[b]
        if state is not None:
            rec = rec + exact_dot(query[b], state, LAST)
            state = state * jnp.exp(total[b, 0:1]) + end[b]
        else:
            state = end[b]
        pay[b, 0:rows, 0:HEAD_DIM] = (rec * gate_out[b]).astype(BF16)
        squares = exact_dot(jnp.ones((16, HEAD_DIM), F32), rec * rec, LAST)
        hi = squares.astype(BF16)
        left = squares - hi.astype(F32)
        mid = left.astype(BF16)
        low = (left - mid.astype(F32)).astype(BF16)
        r = lax.broadcasted_iota(jnp.int32, squares.shape, 0)
        pick = jnp.where(r == 0, hi.astype(F32), jnp.where(r == 1, mid.astype(F32), low.astype(F32)))
        pay[b, rows:, :] = jnp.where(r < 3, pick, 0.0).astype(BF16)
    x = pool_in[...].reshape(blocks * rows, HEAD_DIM)
    pos = lax.broadcasted_iota(jnp.int32, x.shape, 0)
    group = at[1]
    run = x
    window = x
    for level in range(POOL_GROUPS):
        stride = 2**level
        run = run + jnp.where(pos >= stride, pltpu.roll(run, stride, 0), 0.0)
        window = jnp.where(group == level, run, window)
    length = lax.shift_left(jnp.int32(2), group)
    pooled = window / jnp.minimum(pos + 1, length).astype(F32) - x
    pay[:, 0:rows, HEAD_DIM:] = pooled.astype(BF16).reshape(blocks, rows, HEAD_DIM)
    for d in range(N_LINE):
        outs[d][...] = pay[lax.rem(at[0] + d, N_LINE)]


def out_kernel(at, squares, group_weight, pool_gain, *refs):
    pays = refs[:N_LINE]
    weights = refs[N_LINE : 5 * N_LINE]
    keep, give, u, p, norm = refs[5 * N_LINE :]
    place, half_at = at[0], at[1]
    rows = keep.shape[0]
    width = u.shape[1]
    total = 2 * width
    scale = lax.rsqrt(squares[...] / total + EPS)
    norm[...] = jnp.broadcast_to(scale, (HEAD_DIM, scale.shape[1])).T
    sources = (half_at * rows, (1 - half_at) * rows)
    for d in range(N_LINE):
        col = pl.multiple_of(lax.rem(place - d + N_LINE, N_LINE) * HEAD_DIM, HEAD_DIM)
        for h in range(2):
            src = pl.ds(pl.multiple_of(sources[h], rows), rows)
            u[h * rows : (h + 1) * rows, pl.ds(col, HEAD_DIM)] = pays[d][src, 0:HEAD_DIM]
            p[h * rows : (h + 1) * rows, pl.ds(col, HEAD_DIM)] = pays[d][src, HEAD_DIM:]
    groups = width // GROUP_DIM
    for i in range(groups):
        cols = slice(i * GROUP_DIM, (i + 1) * GROUP_DIM)
        mapped = dot(p[:, cols], group_weight[half_at * groups + i])
        p[:, cols] = (mapped * pool_gain[:, cols]).astype(BF16)
    scales = jnp.concatenate(
        [norm[pl.ds(pl.multiple_of(src, rows), rows), :] for src in sources], axis=0
    )
    scales = jnp.concatenate([scales, scales], axis=1)
    for s in range(N_LINE):
        for e in (0, 2):
            first, second = weights[4 * s + e], weights[4 * s + e + 1]
            w_rec = jnp.concatenate([first[0:width], second[0:width]], axis=1)
            w_pool = jnp.concatenate([first[width:], second[width:]], axis=1)
            out = (dot(u[...], w_rec) * scales + dot(p[...], w_pool)).astype(BF16)
            for i in range(2):
                k = at[2 + 4 * s + e + i]
                where = pl.ds(pl.multiple_of(k * HEAD_DIM, HEAD_DIM), HEAD_DIM)
                lanes = slice(i * HEAD_DIM, (i + 1) * HEAD_DIM)
                keep[:, where] = out[0:rows, lanes]
                give[:, where] = out[rows:, lanes]


N_LINE = 4
UP = [(i, i + 1) for i in range(N_LINE - 1)]
DOWN = [(i + 1, i) for i in range(N_LINE - 1)]
SWAP = [(1, 2), (2, 1)]
OUT = [(1, 0), (2, 3)]
CORES = [(0, 1), (1, 0)]


def beside(by):
    return [(i, i ^ by) for i in range(4)]


def spread(x, axis, place):
    from_below = lax.ppermute(x, axis, UP)
    from_above = lax.ppermute(x, axis, DOWN)
    one = place == 1
    second = lax.ppermute(jnp.where(one, from_above, from_below), axis, OUT)
    across = lax.ppermute(jnp.where(one, from_below, from_above), axis, SWAP)
    third = lax.ppermute(across, axis, OUT)
    edge = (place == 0) | (place == N_LINE - 1)
    return (
        x,
        jnp.where(place == 0, from_above, from_below),
        jnp.where(edge, second, from_above),
        jnp.where(edge, third, across),
    )


def call(kernel, outs, in_specs, out_specs, name, scratch=(), aliases=None):
    return pl.pallas_call(
        kernel,
        out_shape=outs,
        in_specs=in_specs,
        out_specs=out_specs,
        scratch_shapes=scratch,
        input_output_aliases=aliases or {},
        name=name,
        compiler_params=pltpu.CompilerParams(vmem_limit_bytes=48 * 2**20),
    )


def fast_body(
    tokens,
    norm_gain,
    w_query,
    forget_weight,
    w_input,
    w_outgate,
    w_pool,
    forget_gap,
    extra_decay,
    rec_gain,
    group_weight,
    pool_gain,
    recurrent_output_weight,
    w_out_pool,
):
    place, line, core = (lax.axis_index(a) for a in ("sp", "fs", "tp"))
    shape = jax.ShapeDtypeStruct
    tok = tokens[0]
    tok_rows, half = tok.shape
    w_rows = w_query.shape[0]
    width = w_query.shape[1]
    wide = 5 * HEAD_DIM
    ints = lambda *v: jnp.stack([jnp.asarray(i, jnp.int32) for i in v])

    pieces = call(
        split_kernel,
        [shape((w_rows, wide), BF16)] * N_LINE,
        [SMEM] + [VMEM] * 5,
        [VMEM] * N_LINE,
        "split",
    )(ints(place), w_query, forget_weight, w_input, w_outgate, w_pool)
    moved = [pieces[0]] + [
        lax.ppermute(pieces[d], "sp", [(i, (i + d) % N_LINE) for i in range(N_LINE)])
        for d in range(1, N_LINE)
    ]
    mine = jnp.stack(moved)
    by_x = lax.ppermute(mine, "fs", beside(1))
    by_y = lax.ppermute(mine, "fs", beside(2))
    cut = N_LINE // 2
    by_xy = jnp.concatenate(
        [
            lax.ppermute(by_x[:cut], "fs", beside(2)),
            lax.ppermute(by_y[cut:], "fs", beside(1)),
        ]
    )
    total_blocks = 4 * N_LINE
    spots = [
        lax.rem(
            lax.rem(place - d + N_LINE, N_LINE) * 4 + (line ^ e) + core * (total_blocks // 2),
            total_blocks,
        )
        for e in range(4)
        for d in range(N_LINE)
    ]
    weight = call(
        place_kernel,
        shape((total_blocks * w_rows, wide), BF16),
        [SMEM] + [ANY] * 4,
        ANY,
        "place",
        scratch=[pltpu.SemaphoreType.DMA((total_blocks,))],
    )(ints(*spots), mine, by_x, by_y, by_xy)

    slots = spread(tok, "sp", place)
    decays = lax.all_gather(extra_decay[0].T, "sp")
    decay = lax.dynamic_index_in_dim(decays, place, 1, False).reshape(-1, 1)
    order = jnp.asarray([[0, 1, 2, 3], [1, 0, 2, 3], [2, 1, 3, 0], [3, 2, 1, 0]], jnp.int32)[place]
    gains = norm_gain.reshape(2, half)
    gains = jnp.where(core == 0, gains, gains[::-1])
    head = lambda v: lax.dynamic_slice_in_dim(v, place * HEAD_DIM, HEAD_DIM, 0)[None]
    gap, gain = head(forget_gap), head(rec_gain)
    sizes = [
        (tok_rows, HEAD_DIM),
        (tok_rows, HEAD_DIM),
        (HEAD_DIM, HEAD_DIM),
        (8, HEAD_DIM),
        (tok_rows, HEAD_DIM),
        (tok_rows, HEAD_DIM),
    ]
    state = []
    for i, slot in enumerate(slots):
        swapped = lax.ppermute(slot, "tp", CORES)
        full = lambda v: pl.BlockSpec(v.shape, lambda g, at: (0, 0))
        operands = [slot, swapped, gains, weight, gap, decay, gain]
        specs = [full(v) for v in operands]
        specs[5] = pl.BlockSpec((tok_rows, 1), lambda g, at: (at[0], 0))
        state = pl.pallas_call(
            block_kernel,
            out_shape=[shape((N_LINE,) + s, F32) for s in sizes],
            grid_spec=pltpu.PrefetchScalarGridSpec(
                num_scalar_prefetch=1,
                grid=(1,),
                in_specs=specs + [ANY] * len(state),
                out_specs=[pl.BlockSpec((1,) + s, lambda g, at: (at[0], 0, 0)) for s in sizes],
            ),
            input_output_aliases={8 + j: j for j in range(len(state))},
            name="block",
            compiler_params=pltpu.CompilerParams(vmem_limit_bytes=48 * 2**20),
        )(lax.dynamic_slice_in_dim(order, i, 1), *operands, *state)

    out_rows = jnp.concatenate([recurrent_output_weight, w_out_pool], axis=0)
    columns = []
    for slot in spread(out_rows, "sp", place):
        columns += [slot] + [lax.ppermute(slot, "fs", beside(e)) for e in (1, 2, 3)]

    heads = width // HEAD_DIM
    group = (core * heads + place) * HEAD_DIM // GROUP_DIM
    pay_rows = tok_rows + 16
    pays = call(
        join_kernel,
        [shape((pay_rows, 2 * HEAD_DIM), BF16)] * N_LINE,
        [SMEM] + [VMEM] * 6,
        [VMEM] * N_LINE,
        "join",
        scratch=[pltpu.VMEM((N_LINE, pay_rows, 2 * HEAD_DIM), BF16)],
    )(ints(place, group), *state)
    got = [pays[0]] + [
        lax.ppermute(pays[d], "sp", [(i, (i + d) % N_LINE) for i in range(N_LINE)])
        for d in range(1, N_LINE)
    ]
    squares = sum(jnp.sum(g[tok_rows : tok_rows + 3].astype(F32), axis=0) for g in got)[None]
    squares = squares + lax.ppermute(squares, "tp", CORES)
    cols = [order[s] * 4 + (line ^ e) for s in range(N_LINE) for e in range(4)]
    d_out = 4 * N_LINE * out_rows.shape[1]
    keep, give = call(
        out_kernel,
        [shape((tok_rows // 2, d_out), BF16)] * 2,
        [SMEM] + [VMEM] * (3 + 5 * N_LINE),
        [VMEM] * 2,
        "out",
        scratch=[
            pltpu.VMEM((tok_rows, width), BF16),
            pltpu.VMEM((tok_rows, width), BF16),
            pltpu.VMEM((tok_rows, HEAD_DIM), F32),
        ],
    )(ints(place, core, *cols), squares, group_weight, pool_gain[None], *got, *columns)
    taken = lax.ppermute(give, "tp", CORES)
    return (keep.astype(F32) + taken.astype(F32)).astype(BF16)[None]


def solution(mesh):
    placed = (
        P("fs", "sp", "tp"),
        P(),
        P(("sp", "fs"), "tp"),
        P(("sp", "fs"), "tp"),
        P(("sp", "fs"), "tp"),
        P(("sp", "fs"), "tp"),
        P(("sp", "fs"), "tp"),
        P("tp"),
        P("fs", "sp", "tp"),
        P("tp"),
        P(),
        P("tp"),
        P("tp", ("sp", "fs")),
        P("tp", ("sp", "fs")),
    )
    sizes = mesh.shape
    by_heads = (sizes["sp"], sizes["fs"], sizes["tp"]) == (N_LINE, 4, 2)
    by_heads = by_heads and D_HGRN == sizes["sp"] * sizes["tp"] * HEAD_DIM
    return jax.shard_map(
        fast_body if by_heads else body, mesh=mesh, in_specs=placed, out_specs=P("fs", ("sp", "tp"), None), check_vma=False
    )
```
